32 devices in a mesh: sp: 4 (over z), fs: 4 (over y, x), tp: 2 (over core).
Axes of the slice: x: 2, y: 2, z: 4, core: 2. Of those that a mesh axis runs over, the one named last changes fastest.
Arguments:
- recurrent_query: bfloat16 [4, 1024, 1024], P('fs', 'sp', 'tp'), may hold values from -6 to 6
- forget_logits: bfloat16 [4, 1024, 1024], P('fs', 'sp', 'tp'), may hold values from -6 to 6
- recurrent_value: bfloat16 [4, 1024, 1024], P('fs', 'sp', 'tp'), may hold values from -6 to 6
- forget_floor: float32 [2, 1024], P(None, 'tp'), may hold values from 0.8 to 1
- extra_log_decay: float32 [4, 1024, 8], P('fs', 'sp', 'tp'), may hold values from -1 to 0
- recurrent_norm_gain: float32 [1024], P('tp'), may hold values from 0.1 to 1.9
- attention_query: bfloat16 [4, 1024, 768], P('fs', 'sp', 'tp'), may hold values from -300 to 300
- latent: bfloat16 [4, 1024, 256], P('fs', 'sp'), may hold values from -6 to 6
- rotary_key: bfloat16 [4, 1024, 32], P('fs', 'sp'), may hold values from -15 to 15
- latent_norm_gain: float32 [256], replicated, may hold values from 0.1 to 1.9
- latent_up_weight: bfloat16 [256, 1024], replicated, may hold values from -0.375 to 0.375
- recurrent_output_weight: bfloat16 [1024, 2048], P('tp', 'fs'), may hold values from -0.1875 to 0.1875
- attention_output_weight: bfloat16 [512, 2048], P('tp', 'fs'), may hold values from -2 to 2
Outputs:
- mixed: bfloat16 [4, 1024, 2048], P('fs', ('sp', 'tp'))
- log_weight: float32 [4, 1024, 8], P('fs', 'sp', 'tp')
The draws below stay inside these ranges and needn't reach their ends.
All inputs are finite; a program needn't handle non-finite values.
Results may differ from the reference program's by a relative error of at most 0.013.
The reference program's roundings to bfloat16 on the way count: a program that leaves them out, or rounds other values in their place, can miss the bound.
Values may be sent and summed in bfloat16 or wider, within the bound.
A program may use at most 128 MiB of HBM per device.

```python
import math
import jax
import jax.numpy as jnp
from jax import lax

D = 2048
RECURRENT_HEADS = 8
HG_DK = 128
HG_DV = 128
MLA_HEADS = 8
NOPE = 64
ROPE = 32
VDIM = 64
KV_RANK = 256
HG_BLOCK = 64
TOK_DEV = 256
SEQUENCE_LENGTH = 1024
SEQUENCE_GROUPS = 4
GROUP_TOKENS = 1024
HG_KEY = 1024
HG_WIDTH = 1024
MLA_WIDTH = 512
N_TP = 2


def draw_forget_floor(key, part):
    pick_key, fast_key, rate_key = jax.random.split(jax.random.fold_in(key, 1), 3)
    slow_share = 0.5
    slowly = jax.random.uniform(pick_key, (2, RECURRENT_HEADS, 1), jnp.float32) < slow_share
    fast_bound = jax.random.uniform(fast_key, (2, RECURRENT_HEADS, HG_DK), jnp.float32, 0.8, 0.92)
    slow_rates = jnp.exp(jax.random.uniform(rate_key, (2, RECURRENT_HEADS, HG_DK), jnp.float32, math.log(0.02), math.log(0.08))) / SEQUENCE_LENGTH
    bounds = jnp.where(slowly, 1.0 - slow_rates, fast_bound)
    return bounds.reshape(2, HG_KEY).astype(jnp.float32)


def draw_extra_log_decay(key, part):
    level_key, striking_key, falling_key = jax.random.split(jax.random.fold_in(key, 2), 3)
    blocks = GROUP_TOKENS // TOK_DEV
    levels = jnp.exp(jax.random.uniform(level_key, (SEQUENCE_GROUPS, blocks, 1, RECURRENT_HEADS), jnp.float32, math.log(0.15), math.log(0.6))) / SEQUENCE_LENGTH
    stable_value = -jnp.broadcast_to(levels, (SEQUENCE_GROUPS, blocks, TOK_DEV, RECURRENT_HEADS)).reshape(SEQUENCE_GROUPS, GROUP_TOKENS, RECURRENT_HEADS)
    spike_strikes = jax.random.uniform(striking_key, (SEQUENCE_GROUPS, GROUP_TOKENS, RECURRENT_HEADS), jnp.float32) < 2.0 / SEQUENCE_LENGTH
    spike_falls = jnp.log(jax.random.uniform(falling_key, (SEQUENCE_GROUPS, GROUP_TOKENS, RECURRENT_HEADS), jnp.float32, 0.5, 0.8))
    return (stable_value + jnp.where(spike_strikes, spike_falls, 0.0)).astype(jnp.float32)


def drawn_keys(key):
    base_keys = jnp.clip(jax.random.normal(jax.random.fold_in(key, 5), (SEQUENCE_GROUPS, GROUP_TOKENS, ROPE), jnp.float32), -4.5, 4.5)
    return base_keys


def draw_rotary_key(key, part):
    base_keys = drawn_keys(key)
    values = base_keys
    return values.astype(jnp.bfloat16)


def draw_attention_query(key, part):
    normal = jnp.clip(2.0 * jax.random.normal(jax.random.fold_in(key, 6), (SEQUENCE_GROUPS, GROUP_TOKENS, MLA_HEADS, NOPE + ROPE), jnp.float32), -12.0, 12.0)
    return normal.reshape(SEQUENCE_GROUPS, GROUP_TOKENS, MLA_HEADS * (NOPE + ROPE)).astype(jnp.bfloat16)


def block_levels(key, extent, pieces, least, largest):
    loudness = 1.0
    for axis_at, shards_of in pieces:
        steps = jax.random.uniform(jax.random.fold_in(jax.random.fold_in(key, 6), axis_at), (shards_of,), jnp.float32, least / len(pieces), largest / len(pieces))
        loudness = loudness * jnp.repeat(jnp.exp(steps), extent[axis_at] // shards_of).reshape((-1,) + (1,) * (len(extent) - 1 - axis_at))
    return loudness


def gaussian(own_key, dims, deviation, limit, pieces=(), kind=jnp.bfloat16):
    entries = jax.random.normal(own_key, dims, jnp.float32) * deviation
    if len(pieces) > 0:
        entries = block_levels(own_key, dims, pieces, -0.22, 0.18) * entries
    return jnp.clip(entries, min=-limit, max=limit).astype(kind)


def setup_inputs(seed: int = 0) -> dict:
    key_of = jax.random.split(jax.random.key(seed), 14)
    recurrent_query = gaussian(key_of[0], (SEQUENCE_GROUPS, GROUP_TOKENS, HG_KEY), 1.0, 6.0, ((0, 4), (1, 4), (2, 2)))
    forget_logits = gaussian(key_of[1], (SEQUENCE_GROUPS, GROUP_TOKENS, HG_KEY), 1.0, 6.0, ((0, 4), (1, 4), (2, 2)))
    recurrent_value = gaussian(key_of[2], (SEQUENCE_GROUPS, GROUP_TOKENS, HG_WIDTH), 1.0, 6.0, ((0, 4), (1, 4), (2, 2)))
    forget_floor = draw_forget_floor(jax.random.fold_in(key_of[13], 71), 0)
    extra_log_decay = draw_extra_log_decay(jax.random.fold_in(key_of[13], 71), 0)
    recurrent_norm_gain = jnp.clip(1.0 + 0.18 * jax.random.normal(key_of[5], (HG_WIDTH,), jnp.float32), 0.1, 1.9)
    attention_query = draw_attention_query(jax.random.fold_in(key_of[13], 71), 0)
    latent = gaussian(key_of[7], (SEQUENCE_GROUPS, GROUP_TOKENS, KV_RANK), 1.0, 6.0, ((0, 4), (1, 4)))
    rotary_key = draw_rotary_key(jax.random.fold_in(key_of[13], 71), 0)
    latent_norm_gain = jnp.clip(1.0 + 0.18 * jax.random.normal(key_of[9], (KV_RANK,), jnp.float32), 0.1, 1.9)
    latent_up_weight = gaussian(key_of[10], (KV_RANK, MLA_HEADS * (NOPE + VDIM)), KV_RANK ** -0.5, 0.375)
    recurrent_output_weight = gaussian(key_of[11], (HG_WIDTH, D), HG_WIDTH ** -0.5, 0.1875, ((0, 2), (1, 4)))
    attention_output_weight = gaussian(key_of[12], (MLA_WIDTH, D), (max(MLA_WIDTH // 64, 1)) ** -0.5, 2.0, ((0, 2), (1, 4)))
    return dict(recurrent_query=recurrent_query, forget_logits=forget_logits, recurrent_value=recurrent_value, forget_floor=forget_floor, extra_log_decay=extra_log_decay, recurrent_norm_gain=recurrent_norm_gain, attention_query=attention_query, latent=latent, rotary_key=rotary_key, latent_norm_gain=latent_norm_gain, latent_up_weight=latent_up_weight, recurrent_output_weight=recurrent_output_weight, attention_output_weight=attention_output_weight)


norm_eps = 1e-06
rope_base = 10000.0
largest_value = lax.Precision.HIGHEST

def rope_tables(token_count, offset):
    places = offset + jnp.arange(token_count).astype(jnp.float32)
    pair_count = ROPE // 2
    inverse = rope_base ** (-jnp.arange(pair_count).astype(jnp.float32) / pair_count)
    angles = places[:, None] * inverse[None, :]
    return (jnp.cos(angles), jnp.sin(angles))

def rotate(tensor, cos_table, sin_table):
    half_width = tensor.shape[-1] // 2
    first_half = tensor[..., :half_width]
    second_half = tensor[..., half_width:]
    return jnp.concatenate([first_half * cos_table - second_half * sin_table, first_half * sin_table + second_half * cos_table], axis=-1)

def block_pass(queries, key_matrix, values, decay_logarithm, carried):
    length = queries.shape[0]
    blocks = length // HG_BLOCK

    def split_blocks(tensor):
        return tensor.reshape((blocks, HG_BLOCK) + tensor.shape[1:])
    lower_mask = jnp.tril(jnp.ones((HG_BLOCK, HG_BLOCK), dtype=bool))

    def advance(running_state, input_tuple):
        query_blk, key_tile, value_tile, decay_blk = input_tuple
        inner_block_term = jnp.cumsum(decay_blk, axis=0)
        damped_query = query_blk * jnp.exp(inner_block_term)
        key_decayed = key_tile * jnp.exp(-inner_block_term)
        cross_block_term = jnp.einsum('mcx,cxn->mcn', damped_query, running_state, precision=largest_value)
        scores = jnp.einsum('thk,shk->hts', damped_query, key_decayed, precision=largest_value)
        scores = jnp.where(lower_mask[None], scores, 0.0)
        intra_term = jnp.einsum('hts,shv->thv', scores, value_tile, precision=largest_value)
        decay_total = inner_block_term[-1]
        updated_state = jnp.exp(decay_total)[:, :, None] * running_state + jnp.einsum('jrg,jrb->rgb', key_tile * jnp.exp(decay_total[None] - inner_block_term), value_tile, precision=largest_value)
        return (updated_state, cross_block_term + intra_term)
    final_state, outputs = lax.scan(advance, carried, (split_blocks(queries), split_blocks(key_matrix), split_blocks(values), split_blocks(decay_logarithm)))
    return (outputs.reshape((length,) + outputs.shape[2:]), final_state)

def gate_factors(forget_gate, spike_amount, gate_floor):
    decay_logarithm = jnp.logaddexp(jnp.log(gate_floor), jnp.log1p(-gate_floor) + jax.nn.log_sigmoid(forget_gate)) + spike_amount[:, :, None]
    key_matrix = (1.0 - gate_floor) * jax.nn.sigmoid(-forget_gate)
    return (key_matrix, decay_logarithm)

def head_norm(outputs, gain):
    return outputs * lax.rsqrt(lax.optimization_barrier(jnp.mean(outputs * outputs, axis=-1, keepdims=True)) + norm_eps) * gain

def recurrence_path(query_rows, forget_input, value_input, spike_amount, forget_floor, recurrent_norm_gain):
    length = query_rows.shape[0]
    queries = query_rows.astype(jnp.float32).reshape(length, RECURRENT_HEADS, HG_DK)
    forget_gate = forget_input.astype(jnp.float32).reshape(length, RECURRENT_HEADS, HG_DK)
    values = value_input.astype(jnp.float32).reshape(length, RECURRENT_HEADS, HG_DV)
    summed = jnp.zeros((length, RECURRENT_HEADS, HG_DV), jnp.float32)
    for direction in range(2):
        gate_floor = forget_floor[direction].reshape(RECURRENT_HEADS, HG_DK)
        key_matrix, decay_logarithm = gate_factors(forget_gate, spike_amount, gate_floor)
        sorted_rows = [queries, key_matrix, values, decay_logarithm]
        if direction == 1:
            sorted_rows = [jnp.flip(member, axis=0) for member in sorted_rows]
        result, unused = block_pass(sorted_rows[0], sorted_rows[1], sorted_rows[2], sorted_rows[3], jnp.zeros((RECURRENT_HEADS, HG_DK, HG_DV), jnp.float32))
        if direction == 1:
            result = jnp.flip(result, axis=0)
        summed = summed + result
    normed = head_norm(summed, recurrent_norm_gain.reshape(RECURRENT_HEADS, HG_DV))
    return normed.astype(jnp.bfloat16).reshape(length, RECURRENT_HEADS * HG_DV)

def attention_branch(query_rows, latent, rotary_key, latent_norm_gain, latent_up_weight):
    length = query_rows.shape[0]
    latent_wide = latent.astype(jnp.float32)
    normed = (latent_wide * lax.rsqrt(lax.optimization_barrier(jnp.mean(latent_wide * latent_wide, axis=-1, keepdims=True)) + norm_eps) * latent_norm_gain).astype(jnp.bfloat16)
    expanded = jnp.dot(normed, latent_up_weight, preferred_element_type=jnp.float32).astype(jnp.bfloat16)
    expanded = expanded.reshape(length, MLA_HEADS, NOPE + VDIM)
    cos_table, sin_table = rope_tables(length, 0.0)
    rotated_key = rotate(rotary_key.astype(jnp.float32), cos_table, sin_table).astype(jnp.bfloat16)
    head_query = query_rows.reshape(length, MLA_HEADS, NOPE + ROPE)
    query_rope = rotate(head_query[..., NOPE:].astype(jnp.float32), cos_table[:, None], sin_table[:, None])
    query_all = jnp.concatenate([head_query[..., :NOPE], query_rope.astype(jnp.bfloat16)], axis=-1)
    keys_all = jnp.concatenate([expanded[..., :NOPE], jnp.broadcast_to(rotated_key[:, None, :], (length, MLA_HEADS, ROPE))], axis=-1)
    values = expanded[..., NOPE:].astype(jnp.float32)
    keys_wide = keys_all.astype(jnp.float32)
    score_scale = (NOPE + ROPE) ** (-0.5)
    rows_block = min(length, 512)

    def one_block(query_block):
        scores = jnp.einsum('qhd,khd->hqk', query_block.astype(jnp.float32), keys_wide) * score_scale
        row_peak = lax.optimization_barrier(jnp.max(scores, axis=-1))
        weights = jnp.exp(scores - row_peak[..., None])
        totals = lax.optimization_barrier(jnp.sum(weights, axis=-1))
        rounded = lax.optimization_barrier(weights.astype(jnp.bfloat16)).astype(jnp.float32)
        weighted = jnp.einsum('hqk,khv->qhv', rounded, values) / totals.T[:, :, None]
        return (weighted.astype(jnp.bfloat16).reshape(rows_block, MLA_HEADS * VDIM), (row_peak + jnp.log(totals)).T)
    outputs, log_weight = lax.map(one_block, query_all.reshape(length // rows_block, rows_block, MLA_HEADS, NOPE + ROPE))
    return (outputs.reshape(length, MLA_HEADS * VDIM), log_weight.reshape(length, MLA_HEADS))

def reference(recurrent_query, forget_logits, recurrent_value, forget_floor, extra_log_decay, recurrent_norm_gain, attention_query, latent, rotary_key, latent_norm_gain, latent_up_weight, recurrent_output_weight, attention_output_weight):
    seq_count = SEQUENCE_GROUPS * (GROUP_TOKENS // SEQUENCE_LENGTH)

    def sequence_view(tensor):
        return tensor.reshape(seq_count, SEQUENCE_LENGTH, tensor.shape[-1])
    recurrence_result = lax.map(lambda input_tuple: recurrence_path(input_tuple[0], input_tuple[1], input_tuple[2], input_tuple[3], forget_floor, recurrent_norm_gain), (sequence_view(recurrent_query), sequence_view(forget_logits), sequence_view(recurrent_value), sequence_view(extra_log_decay)))
    attended, log_weight = lax.map(lambda input_tuple: attention_branch(input_tuple[0], input_tuple[1], input_tuple[2], latent_norm_gain, latent_up_weight), (sequence_view(attention_query), sequence_view(latent), sequence_view(rotary_key)))
    rows_total = SEQUENCE_GROUPS * GROUP_TOKENS
    recurrence_result = recurrence_result.reshape(rows_total, HG_WIDTH)
    attended = attended.reshape(rows_total, MLA_WIDTH)
    hg_share = HG_WIDTH // N_TP
    att_share = MLA_WIDTH // N_TP
    summed = jnp.zeros((rows_total, D), jnp.float32)
    for tp_half in range(N_TP):
        partial_term = jnp.dot(recurrence_result[:, tp_half * hg_share:(tp_half + 1) * hg_share], recurrent_output_weight[tp_half * hg_share:(tp_half + 1) * hg_share], preferred_element_type=jnp.float32)
        partial_term = partial_term + jnp.dot(attended[:, tp_half * att_share:(tp_half + 1) * att_share], attention_output_weight[tp_half * att_share:(tp_half + 1) * att_share], preferred_element_type=jnp.float32)
        summed = summed + lax.optimization_barrier(partial_term.astype(jnp.bfloat16)).astype(jnp.float32)
    mixed = summed.astype(jnp.bfloat16).reshape(SEQUENCE_GROUPS, GROUP_TOKENS, D)
    return (mixed, log_weight.reshape(SEQUENCE_GROUPS, GROUP_TOKENS, MLA_HEADS))
```

```python
import functools

import jax
import jax.numpy as jnp
import numpy as np
from jax import lax
from jax.experimental import pallas as pl
from jax.experimental.pallas import tpu as pltpu
from jax.sharding import PartitionSpec as P

HG_DK = 128
NOPE = 64
ROPE = 32
VDIM = 64
HEAD = NOPE + ROPE
LANES = 128
BLOCK = 128
DECAY_ROWS = 16

norm_eps = 1e-06
rope_base = 10000.0
widest_span = 8

F32 = jnp.float32
BF16 = jnp.bfloat16


def mm(a, b):
    return jnp.dot(a, b, preferred_element_type=F32)


def mm_nt(a, b):
    return lax.dot_general(a, b, (((1,), (1,)), ((), ())), preferred_element_type=F32)


def mm_tn(a, b):
    return lax.dot_general(a, b, (((0,), (0,)), ((), ())), preferred_element_type=F32)


def rope_constants(seq_len, heads):
    half = ROPE // 2
    inverse = (np.float32(rope_base) ** (-np.arange(half, dtype=np.float32) / np.float32(half))).astype(np.float32)
    angles = np.arange(seq_len, dtype=np.float32)[:, None] * inverse[None, :]
    cos_pad = np.zeros((seq_len, LANES), np.float32)
    sin_pad = np.zeros((seq_len, LANES), np.float32)
    cos_pad[:, :NOPE] = 1.0
    cos_pad[:, NOPE:HEAD] = np.tile(np.cos(angles), (1, 2))
    sin_pad[:, NOPE:HEAD] = np.tile(np.sin(angles), (1, 2))
    place = np.zeros((heads * HEAD, heads * LANES), np.float32)
    swap = np.zeros((heads * HEAD, heads * LANES), np.float32)
    for h in range(heads):
        for i in range(HEAD):
            place[h * HEAD + i, h * LANES + i] = 1.0
        for i in range(half):
            a, b = NOPE + i, NOPE + half + i
            swap[h * HEAD + b, h * LANES + a] = -1.0
            swap[h * HEAD + a, h * LANES + b] = 1.0
    return cos_pad, sin_pad, place, swap


def kernel(
    sizes,
    q_ref, f_ref, v_ref, floor_ref, extra_ref, gain_ref, aq_ref, lat_ref, rk_ref,
    lgain_ref, wup_ref, cos_ref, sin_ref, place_ref, swap_ref, w1_ref, w2_ref,
    out_ref, logw_ref,
    lbuf, ssend, srecv, w1buf, w2buf, psend, precv,
    kbuf, vbuf, intra, qf_ref, qb_ref, sf_ref, sb_ref, act,
    l_send, l_recv, s_send, s_recv, w_send, w_recv, x_send, x_recv, own_sem,
):
    n_fs, span = sizes
    tokens, width = q_ref.shape
    heads = width // HG_DK
    att_heads = aq_ref.shape[1] // HEAD
    up = att_heads * (NOPE + VDIM)
    blocks = tokens // BLOCK
    latent_width = lat_ref.shape[1]
    columns = w1_ref.shape[1]
    rows = tokens // 2

    sp, fs, tp = lax.axis_index("sp"), lax.axis_index("fs"), lax.axis_index("tp")
    place = lax.rem(sp, span)
    base = sp - place

    def sp_peer(j):
        return {"sp": base + lax.rem(place + j, span)}

    def fs_peer(j):
        return {"fs": lax.rem(fs + j, n_fs)}

    partner = {"tp": 1 - tp}

    barrier = pltpu.get_barrier_semaphore()
    for j in range(1, n_fs):
        pl.semaphore_signal(barrier, inc=1, device_id=fs_peer(j), device_id_type=pl.DeviceIdType.MESH)
    for j in range(1, span):
        pl.semaphore_signal(barrier, inc=1, device_id=sp_peer(j), device_id_type=pl.DeviceIdType.MESH)
    pl.semaphore_signal(barrier, inc=1, device_id=partner, device_id_type=pl.DeviceIdType.MESH)
    pl.semaphore_wait(barrier, n_fs + span - 1)

    def remote(src, dst, send, recv, device):
        return pltpu.make_async_remote_copy(
            src_ref=src, dst_ref=dst, send_sem=send, recv_sem=recv,
            device_id=device, device_id_type=pl.DeviceIdType.MESH,
        )

    w_copies = []
    for j in range(1, n_fs):
        pair = (
            remote(w1_ref, w1buf.at[j], w_send.at[2 * j], w_recv.at[2 * j], fs_peer(j)),
            remote(w2_ref, w2buf.at[j], w_send.at[2 * j + 1], w_recv.at[2 * j + 1], fs_peer(j)),
        )
        for c in pair:
            c.start()
        w_copies.append(pair)
    own = (
        pltpu.make_async_copy(w1_ref, w1buf.at[0], own_sem.at[0]),
        pltpu.make_async_copy(w2_ref, w2buf.at[0], own_sem.at[1]),
    )
    for c in own:
        c.start()

    offset = pl.multiple_of(place * tokens, tokens)
    cos = cos_ref[pl.ds(offset, tokens), :]
    sin = sin_ref[pl.ds(offset, tokens), :]
    lat = lat_ref[...].astype(F32)
    normed = lat * lax.rsqrt(jnp.mean(lat * lat, axis=-1, keepdims=True) + norm_eps) * lgain_ref[...]
    lbuf[0, :, :latent_width] = normed.astype(BF16)
    rk = rk_ref[...]
    rotated = mm(rk, place_ref[NOPE:HEAD, :LANES]) * cos + mm(rk, swap_ref[NOPE:HEAD, :LANES]) * sin
    lbuf[0, :, latent_width:] = rotated.astype(BF16)
    l_copies = []
    for j in range(1, span):
        c = remote(lbuf.at[0], lbuf.at[j], l_send.at[j], l_recv.at[j], sp_peer(j))
        c.start()
        l_copies.append(c)

    row = lax.broadcasted_iota(jnp.int32, (BLOCK, BLOCK), 0)
    col = lax.broadcasted_iota(jnp.int32, (BLOCK, BLOCK), 1)
    lower = row >= col
    upper = row <= col
    tri = (jnp.where(lower, 1.0, 0.0).astype(BF16), jnp.where(upper, 1.0, 0.0).astype(BF16))
    block_decay = [[[None] * blocks for _ in range(2)] for _ in range(heads)]
    for h in range(heads):
        lanes = slice(h * HG_DK, (h + 1) * HG_DK)
        for b in range(blocks):
            tok = slice(b * BLOCK, (b + 1) * BLOCK)
            q = q_ref[tok, lanes].astype(F32)
            gate = f_ref[tok, lanes].astype(F32)
            v = v_ref[tok, lanes]
            miss = 1.0 / (1.0 + jnp.exp(gate))
            spike = extra_ref[tok, h : h + 1]
            scores = None
            for d in range(2):
                keyed = (1.0 - floor_ref[d : d + 1, lanes]) * miss
                decay = jnp.log1p(-keyed) + spike
                hi = decay.astype(BF16)
                lo = (decay - hi.astype(F32)).astype(BF16)
                run = mm(tri[d], hi) + mm(tri[d], lo)
                mid_at = BLOCK // 2 - 1 if d == 0 else BLOCK // 2
                end_at = BLOCK - 1 if d == 0 else 0
                mid = run[mid_at : mid_at + 1]
                end = run[end_at : end_at + 1]
                grow = jnp.exp(run - mid)
                qd = q * grow
                kd = keyed * jnp.exp(mid - run)
                s = mm_nt(qd.astype(BF16), kd.astype(BF16))
                s = jnp.where(lower if d == 0 else upper, s, 0.0)
                scores = s if scores is None else scores + s
                cross = qf_ref if d == 0 else qb_ref
                cross[tok, lanes] = (qd * jnp.exp(mid)).astype(BF16)
                state = mm_tn(v, (kd * jnp.exp(end - mid)).astype(BF16))
                keep = sf_ref if d == 0 else sb_ref
                keep[b, :, lanes] = state
                block_decay[h][d][b] = jnp.exp(end)
            intra[tok, lanes] = mm(scores.astype(BF16), v)
        for d in range(2):
            keep = sf_ref if d == 0 else sb_ref
            order = range(blocks) if d == 0 else range(blocks - 1, -1, -1)
            total, decay_all = None, None
            for b in order:
                one = keep[b, :, lanes]
                dec = block_decay[h][d][b]
                total = one if total is None else total * dec + one
                decay_all = dec if decay_all is None else decay_all * dec
            ssend[d, :HG_DK, lanes] = total.astype(BF16)
            ssend[d, HG_DK:, lanes] = jnp.broadcast_to(decay_all, (DECAY_ROWS, HG_DK)).astype(BF16)
    s_copies = []
    for j in range(1, span):
        which = jnp.where(place + j < span, 0, 1)
        c = remote(ssend.at[which], srecv.at[j], s_send.at[j], s_recv.at[j], sp_peer(j))
        c.start()
        s_copies.append(c)

    tp_up = pl.multiple_of(tp * up, LANES)
    wup = wup_ref[:, pl.ds(tp_up, up)]
    lane = lax.broadcasted_iota(jnp.int32, (tokens, LANES), 1)
    for j in range(span):
        if j > 0:
            l_copies[j - 1].wait_recv()
        keys = slice(j * tokens, (j + 1) * tokens)
        expanded = mm(lbuf[j, :, :latent_width], wup)
        rot = lbuf[j, :, latent_width:].astype(F32)
        vbuf[keys, :] = expanded.astype(BF16)
        for h in range(att_heads):
            lanes = slice(h * LANES, (h + 1) * LANES)
            kbuf[keys, lanes] = jnp.where(lane < NOPE, expanded[:, lanes], rot).astype(BF16)
    aq = aq_ref[...]
    scale = HEAD ** (-0.5)
    head_lane = lax.broadcasted_iota(jnp.int32, (tokens, att_heads), 1)
    logw = jnp.zeros((tokens, att_heads), F32)
    kept = None
    for h in range(att_heads):
        lanes = slice(h * LANES, (h + 1) * LANES)
        query = mm(aq, place_ref[:, lanes]) * cos + mm(aq, swap_ref[:, lanes]) * sin
        scores = mm_nt(query.astype(BF16), kbuf[:, lanes]) * scale
        peak = jnp.max(scores, axis=-1, keepdims=True)
        weights = jnp.exp(scores - peak)
        totals = jnp.sum(weights, axis=-1, keepdims=True)
        result = mm(weights.astype(BF16), vbuf[:, lanes]) / totals
        logw = jnp.where(head_lane == h, peak + jnp.log(totals), logw)
        if h % 2 == 0:
            kept = pltpu.roll(result, VDIM, 1)
        else:
            at = width + (h // 2) * LANES
            act[:, at : at + LANES] = jnp.where(lane < VDIM, kept, result).astype(BF16)
    logw_ref[...] = logw

    for c in s_copies:
        c.wait_recv()
    for h in range(heads):
        lanes = slice(h * HG_DK, (h + 1) * HG_DK)
        carry_f = jnp.zeros((HG_DK, HG_DK), F32)
        carry_b = jnp.zeros((HG_DK, HG_DK), F32)
        for j in range(span - 1, 0, -1):
            new = carry_f * srecv[j, HG_DK : HG_DK + 1, lanes].astype(F32) + srecv[j, :HG_DK, lanes].astype(F32)
            carry_f = jnp.where(j <= place, new, carry_f)
        for j in range(1, span):
            new = carry_b * srecv[j, HG_DK : HG_DK + 1, lanes].astype(F32) + srecv[j, :HG_DK, lanes].astype(F32)
            carry_b = jnp.where(j > place, new, carry_b)
        starts_f = []
        for b in range(blocks):
            starts_f.append(carry_f)
            carry_f = carry_f * block_decay[h][0][b] + sf_ref[b, :, lanes]
        starts_b = [None] * blocks
        for b in range(blocks - 1, -1, -1):
            starts_b[b] = carry_b
            carry_b = carry_b * block_decay[h][1][b] + sb_ref[b, :, lanes]
        for b in range(blocks):
            tok = slice(b * BLOCK, (b + 1) * BLOCK)
            o = intra[tok, lanes]
            o = o + mm_nt(qf_ref[tok, lanes], starts_f[b].astype(BF16))
            o = o + mm_nt(qb_ref[tok, lanes], starts_b[b].astype(BF16))
            o = o * lax.rsqrt(jnp.mean(o * o, axis=-1, keepdims=True) + norm_eps) * gain_ref[:, lanes]
            act[tok, lanes] = o.astype(BF16)

    mine = pl.multiple_of(tp * rows, rows)
    theirs = pl.multiple_of((1 - tp) * rows, rows)
    kept_rows = []
    x_copies = []

    def finish(j):
        x_copies[j].wait_recv()
        at = pl.multiple_of(lax.rem(fs - j + n_fs, n_fs) * columns, LANES)
        out_ref[:, pl.ds(at, columns)] = (kept_rows[j] + precv[j].astype(F32)).astype(BF16)

    for j in range(n_fs):
        if j == 0:
            for c in own:
                c.wait()
        else:
            for c in w_copies[j - 1]:
                c.wait_recv()
        away = mm(act[pl.ds(theirs, rows), :width], w1buf[j]) + mm(act[pl.ds(theirs, rows), width:], w2buf[j])
        psend[j] = away.astype(BF16)
        c = remote(psend.at[j], precv.at[j], x_send.at[j], x_recv.at[j], partner)
        c.start()
        x_copies.append(c)
        here = mm(act[pl.ds(mine, rows), :width], w1buf[j]) + mm(act[pl.ds(mine, rows), width:], w2buf[j])
        kept_rows.append(here.astype(BF16).astype(F32))
        if j > 0:
            finish(j - 1)
    finish(n_fs - 1)

    for pair in w_copies:
        for c in pair:
            c.wait_send()
    for c in l_copies + s_copies + x_copies:
        c.wait_send()


def local(
    n_fs,
    n_sp,
    recurrent_query,
    forget_logits,
    recurrent_value,
    forget_floor,
    extra_log_decay,
    recurrent_norm_gain,
    attention_query,
    latent,
    rotary_key,
    latent_norm_gain,
    latent_up_weight,
    recurrent_output_weight,
    attention_output_weight,
):
    span = min(n_sp, widest_span)
    tokens, width = recurrent_query.shape[1:]
    heads = width // HG_DK
    att_heads = attention_query.shape[2] // HEAD
    latent_width = latent.shape[2]
    columns = recurrent_output_weight.shape[1]
    att_width = attention_output_weight.shape[0]
    blocks = tokens // BLOCK
    rows = tokens // 2
    cos_pad, sin_pad, place, swap = rope_constants(span * tokens, att_heads)
    vmem = pl.BlockSpec(memory_space=pltpu.VMEM)
    anywhere = pl.BlockSpec(memory_space=pl.ANY)
    dma = pltpu.SemaphoreType.DMA
    mixed, log_weight = pl.pallas_call(
        functools.partial(kernel, (n_fs, span)),
        out_shape=(
            jax.ShapeDtypeStruct((rows, columns * n_fs), BF16),
            jax.ShapeDtypeStruct((tokens, att_heads), F32),
        ),
        in_specs=[vmem] * 15 + [anywhere] * 2,
        out_specs=(vmem, vmem),
        scratch_shapes=[
            pltpu.VMEM((span, tokens, latent_width + LANES), BF16),
            pltpu.VMEM((2, HG_DK + DECAY_ROWS, width), BF16),
            pltpu.VMEM((span, HG_DK + DECAY_ROWS, width), BF16),
            pltpu.VMEM((n_fs, width, columns), BF16),
            pltpu.VMEM((n_fs, att_width, columns), BF16),
            pltpu.VMEM((n_fs, rows, columns), BF16),
            pltpu.VMEM((n_fs, rows, columns), BF16),
            pltpu.VMEM((span * tokens, att_heads * LANES), BF16),
            pltpu.VMEM((span * tokens, att_heads * LANES), BF16),
            pltpu.VMEM((tokens, width), F32),
            pltpu.VMEM((tokens, width), BF16),
            pltpu.VMEM((tokens, width), BF16),
            pltpu.VMEM((blocks, HG_DK, width), F32),
            pltpu.VMEM((blocks, HG_DK, width), F32),
            pltpu.VMEM((tokens, width + att_width), BF16),
            dma((span,)), dma((span,)), dma((span,)), dma((span,)),
            dma((2 * n_fs,)), dma((2 * n_fs,)), dma((n_fs,)), dma((n_fs,)), dma((2,)),
        ],
        compiler_params=pltpu.CompilerParams(
            collective_id=0, has_side_effects=True, vmem_limit_bytes=56 * 2**20
        ),
        name="mixers",
    )(
        recurrent_query[0],
        forget_logits[0],
        recurrent_value[0],
        forget_floor,
        extra_log_decay[0],
        recurrent_norm_gain[None],
        attention_query[0],
        latent[0],
        rotary_key[0],
        latent_norm_gain[None],
        latent_up_weight,
        jnp.asarray(cos_pad),
        jnp.asarray(sin_pad),
        jnp.asarray(place, BF16),
        jnp.asarray(swap, BF16),
        recurrent_output_weight,
        attention_output_weight,
    )
    return mixed[None], log_weight[None]


def solution(mesh):
    placed = (
        P("fs", "sp", "tp"),
        P("fs", "sp", "tp"),
        P("fs", "sp", "tp"),
        P(None, "tp"),
        P("fs", "sp", "tp"),
        P("tp"),
        P("fs", "sp", "tp"),
        P("fs", "sp", None),
        P("fs", "sp", None),
        P(),
        P(),
        P("tp", "fs"),
        P("tp", "fs"),
    )
    return jax.shard_map(
        functools.partial(local, mesh.shape["fs"], mesh.shape["sp"]),
        mesh=mesh,
        in_specs=placed,
        out_specs=(P("fs", ("sp", "tp"), None), P("fs", "sp", "tp")),
        check_vma=False,
    )
```

```python
import functools

import jax
import jax.numpy as jnp
import numpy as np
from jax import lax
from jax.experimental import pallas as pl
from jax.experimental.pallas import tpu as pltpu
from jax.sharding import PartitionSpec as P

HG_DK = 128
NOPE = 64
ROPE = 32
VDIM = 64
HEAD = NOPE + ROPE
LANES = 128
BLOCK = 128

norm_eps = 1e-06
rope_base = 10000.0
widest_span = 8

F32 = jnp.float32
BF16 = jnp.bfloat16


def mm(a, b):
    return jnp.dot(a, b, preferred_element_type=F32)


def mm_nt(a, b):
    return lax.dot_general(a, b, (((1,), (1,)), ((), ())), preferred_element_type=F32)


def mm_tn(a, b):
    return lax.dot_general(a, b, (((0,), (0,)), ((), ())), preferred_element_type=F32)


def flip_bits(value, mask):
    bit = 1
    while bit <= mask:
        if mask & bit:
            value = value + bit - 2 * bit * lax.rem(value // bit, 2)
        bit *= 2
    return value


def rope_constants(seq_len, heads):
    half = ROPE // 2
    inverse = (np.float32(rope_base) ** (-np.arange(half, dtype=np.float32) / np.float32(half))).astype(np.float32)
    angles = np.arange(seq_len, dtype=np.float32)[:, None] * inverse[None, :]
    cos_pad = np.zeros((seq_len, LANES), np.float32)
    sin_pad = np.zeros((seq_len, LANES), np.float32)
    cos_pad[:, :NOPE] = 1.0
    cos_pad[:, NOPE:HEAD] = np.tile(np.cos(angles), (1, 2))
    sin_pad[:, NOPE:HEAD] = np.tile(np.sin(angles), (1, 2))
    place = np.zeros((heads * HEAD, heads * LANES), np.float32)
    swap = np.zeros((heads * HEAD, heads * LANES), np.float32)
    for h in range(heads):
        for i in range(HEAD):
            place[h * HEAD + i, h * LANES + i] = 1.0
        for i in range(half):
            a, b = NOPE + i, NOPE + half + i
            swap[h * HEAD + b, h * LANES + a] = -1.0
            swap[h * HEAD + a, h * LANES + b] = 1.0
    return cos_pad, sin_pad, place, swap


def kernel(
    sizes,
    q_ref, f_ref, v_ref, floor_ref, extra_ref, gain_ref, aq_ref, lat_ref, rk_ref,
    lgain_ref, wup_ref, cos_ref, sin_ref, place_ref, swap_ref, w1_ref, w2_ref,
    out_ref, logw_ref,
    lbuf, ssend, srecv, w1buf, w2buf, psend, precv,
    kbuf, vbuf, intra, qf_ref, qb_ref, sf_ref, sb_ref, act, whole_state, whole_decay,
    l_send, l_recv, f_send, f_recv, s_send, s_recv, w_send, w_recv, r_send, r_recv,
    x_send, x_recv, own_sem,
):
    n_fs, span = sizes
    tokens, width = q_ref.shape
    heads = width // HG_DK
    att_heads = aq_ref.shape[1] // HEAD
    up = att_heads * (NOPE + VDIM)
    blocks = tokens // BLOCK
    latent_width = lat_ref.shape[1]
    columns = w1_ref.shape[1]
    rows = tokens // 2

    sp, fs, tp = lax.axis_index("sp"), lax.axis_index("fs"), lax.axis_index("tp")
    place = lax.rem(sp, span)
    base = sp - place

    def sp_peer(j):
        return {"sp": base + lax.rem(place + j, span)}

    def fs_peer(j):
        return {"fs": flip_bits(fs, j)}

    partner = {"tp": 1 - tp}

    barrier = pltpu.get_barrier_semaphore()
    for j in range(1, n_fs):
        pl.semaphore_signal(barrier, inc=1, device_id=fs_peer(j), device_id_type=pl.DeviceIdType.MESH)
    for j in range(1, span):
        pl.semaphore_signal(barrier, inc=1, device_id=sp_peer(j), device_id_type=pl.DeviceIdType.MESH)
    pl.semaphore_signal(barrier, inc=1, device_id=partner, device_id_type=pl.DeviceIdType.MESH)
    pl.semaphore_wait(barrier, n_fs + span - 1)

    def remote(src, dst, send, recv, device):
        return pltpu.make_async_remote_copy(
            src_ref=src, dst_ref=dst, send_sem=send, recv_sem=recv,
            device_id=device, device_id_type=pl.DeviceIdType.MESH,
        )

    parity = lax.rem(place, 2)
    pair = {"sp": base + flip_bits(place, 1)}
    far = [j for j in range(1, n_fs) if j & (j - 1) and span % 2 == 0]
    near = [j for j in range(1, n_fs) if j not in far]
    weights = ((w1_ref, w1buf), (w2_ref, w2buf))

    def half_rows(ref):
        size = ref.shape[-2] // 2
        return pl.ds(pl.multiple_of(parity * size, size), size)

    w_copies = {}
    for j in far + near:
        pieces = []
        for k, (src, dst) in enumerate(weights):
            there = dst.at[j]
            if j in far:
                src, there = src.at[half_rows(src)], there.at[half_rows(dst)]
            c = remote(src, there, w_send.at[2 * j + k], w_recv.at[2 * j + k], fs_peer(j))
            c.start()
            pieces.append(c)
        w_copies[j] = pieces
    relays = {j: [
        remote(dst.at[j, half_rows(dst)], dst.at[j, half_rows(dst)],
               r_send.at[2 * j + k], r_recv.at[2 * j + k], pair)
        for k, (_, dst) in enumerate(weights)
    ] for j in far}
    own = (
        pltpu.make_async_copy(w1_ref, w1buf.at[0], own_sem.at[0]),
        pltpu.make_async_copy(w2_ref, w2buf.at[0], own_sem.at[1]),
    )
    for c in own:
        c.start()

    offset = pl.multiple_of(place * tokens, tokens)
    cos = cos_ref[pl.ds(offset, tokens), :]
    sin = sin_ref[pl.ds(offset, tokens), :]
    lat = lat_ref[...].astype(F32)
    normed = lat * lax.rsqrt(jnp.mean(lat * lat, axis=-1, keepdims=True) + norm_eps) * lgain_ref[...]
    lbuf[0, :, :latent_width] = normed.astype(BF16)
    rk = rk_ref[...]
    rotated = mm_tn(rk, place_ref[NOPE:HEAD, :LANES]) * cos + mm_tn(rk, swap_ref[NOPE:HEAD, :LANES]) * sin
    lbuf[0, :, latent_width:] = rotated.astype(BF16)
    my_rows = pl.ds(pl.multiple_of(tp * rows, rows), rows)
    l_copies = []
    for j in range(1, span):
        c = remote(lbuf.at[0, my_rows], lbuf.at[j, my_rows], l_send.at[j], l_recv.at[j], sp_peer(j))
        c.start()
        l_copies.append(c)

    row = lax.broadcasted_iota(jnp.int32, (BLOCK, BLOCK), 0)
    col = lax.broadcasted_iota(jnp.int32, (BLOCK, BLOCK), 1)
    lower = row >= col
    upper = row <= col
    tri = (jnp.where(lower, 1.0, 0.0).astype(BF16), jnp.where(upper, 1.0, 0.0).astype(BF16))
    spikes = lax.dot_general(
        extra_ref[...],
        jnp.where(
            lax.broadcasted_iota(jnp.int32, (heads, width), 0)
            == lax.broadcasted_iota(jnp.int32, (heads, width), 1) // HG_DK, 1.0, 0.0),
        (((0,), (0,)), ((), ())), precision=lax.Precision.HIGHEST, preferred_element_type=F32)
    block_decay = [[[None] * blocks for _ in range(2)] for _ in range(heads)]
    for h in range(heads):
        lanes = slice(h * HG_DK, (h + 1) * HG_DK)
        for b in range(blocks):
            tok = slice(b * BLOCK, (b + 1) * BLOCK)
            q = q_ref[tok, lanes].astype(F32)
            gate = f_ref[tok, lanes].astype(F32)
            v = v_ref[tok, lanes]
            miss = 1.0 / (1.0 + jnp.exp(gate))
            spike = spikes[tok, lanes]
            scores = None
            for d in range(2):
                keyed = (1.0 - floor_ref[d : d + 1, lanes]) * miss
                decay = jnp.log1p(-keyed) + spike
                hi = decay.astype(BF16)
                lo = (decay - hi.astype(F32)).astype(BF16)
                run = mm(tri[d], hi) + mm(tri[d], lo)
                mid_at = BLOCK // 2 - 1 if d == 0 else BLOCK // 2
                end_at = BLOCK - 1 if d == 0 else 0
                mid = run[mid_at : mid_at + 1]
                end = run[end_at : end_at + 1]
                grow = jnp.exp(run - mid)
                qd = q * grow
                kd = keyed * jnp.exp(mid - run)
                s = mm_nt(qd.astype(BF16), kd.astype(BF16))
                s = jnp.where(lower if d == 0 else upper, s, 0.0)
                scores = s if scores is None else scores + s
                cross = qf_ref if d == 0 else qb_ref
                cross[tok, lanes] = (qd * jnp.exp(mid)).astype(BF16)
                state = mm_tn(v, (kd * jnp.exp(end - mid)).astype(BF16))
                keep = sf_ref if d == 0 else sb_ref
                keep[b, :, lanes] = state
                block_decay[h][d][b] = jnp.exp(end)
            intra[tok, lanes] = mm(scores.astype(BF16), v)
        for d in range(2):
            keep = sf_ref if d == 0 else sb_ref
            order = range(blocks) if d == 0 else range(blocks - 1, -1, -1)
            total, decay_all = None, None
            for b in order:
                one = keep[b, :, lanes]
                dec = block_decay[h][d][b]
                total = one if total is None else total * dec + one
                decay_all = dec if decay_all is None else decay_all * dec
            whole_state[d, h] = total
            whole_decay[d, h] = jnp.broadcast_to(decay_all, (8, HG_DK))

    first = jnp.where(2 * place < span, 0, 1)

    def link(d, h):
        towards = jnp.clip(place + 1 - 2 * d, 0, span - 1)
        return remote(ssend.at[d, h], srecv.at[d, h], s_send.at[d, h], s_recv.at[d, h],
                      {"sp": base + towards})

    def has_previous(d):
        return jnp.where(d == 0, place, span - 1 - place) > 0

    def has_next(d):
        return jnp.where(d == 0, span - 1 - place, place) > 0

    def pass_on(d):
        for h in range(heads):
            @pl.when(has_previous(d))
            def _():
                link(d, h).wait_recv()

            @pl.when(jnp.logical_not(has_previous(d)))
            def _():
                srecv[d, h] = jnp.zeros((HG_DK, HG_DK), BF16)

            @pl.when(has_next(d))
            def _():
                reached = srecv[d, h].astype(F32) * whole_decay[d, h, 0:1] + whole_state[d, h]
                ssend[d, h] = reached.astype(BF16)
                link(d, h).start()

    pass_on(first)

    forwards = []
    for j in range(1, span):
        l_copies[j - 1].wait_recv()
        c = remote(lbuf.at[j, my_rows], lbuf.at[j, my_rows], f_send.at[j], f_recv.at[j], partner)
        c.start()
        forwards.append(c)

    @pl.when(has_next(1 - first))
    def _():
        pass_on(1 - first)

    for j in far:
        for c, r in zip(w_copies[j], relays[j]):
            c.wait_recv()
            r.start()

    tp_up = pl.multiple_of(tp * up, LANES)
    wup = wup_ref[:, pl.ds(tp_up, up)]
    lane = lax.broadcasted_iota(jnp.int32, (tokens, LANES), 1)
    for j in range(span):
        if j > 0:
            forwards[j - 1].wait_recv()
        keys = slice(j * tokens, (j + 1) * tokens)
        expanded = mm(lbuf[j, :, :latent_width], wup)
        rot = lbuf[j, :, latent_width:].astype(F32)
        vbuf[keys, :] = expanded.astype(BF16)
        for h in range(att_heads):
            lanes = slice(h * LANES, (h + 1) * LANES)
            kbuf[keys, lanes] = jnp.where(lane < NOPE, expanded[:, lanes], rot).astype(BF16)
    aq = aq_ref[...]
    scale = HEAD ** (-0.5)
    logw = jnp.zeros((tokens, LANES), F32)
    kept = None
    for h in range(att_heads):
        lanes = slice(h * LANES, (h + 1) * LANES)
        query = mm(aq, place_ref[:, lanes]) * cos + mm(aq, swap_ref[:, lanes]) * sin
        scores = mm_nt(query.astype(BF16), kbuf[:, lanes]) * scale
        peak = jnp.max(scores, axis=-1, keepdims=True)
        weights = jnp.exp(scores - peak)
        totals = jnp.sum(weights, axis=-1, keepdims=True)
        result = mm(weights.astype(BF16), vbuf[:, lanes]) / totals
        logw = jnp.where(lane == h, peak + jnp.log(totals), logw)
        if h % 2 == 0:
            kept = pltpu.roll(result, VDIM, 1)
        else:
            at = width + (h // 2) * LANES
            act[:, at : at + LANES] = jnp.where(lane < VDIM, kept, result).astype(BF16)
    logw_ref[...] = jnp.transpose(logw)[:att_heads]

    @pl.when(jnp.logical_not(has_next(1 - first)))
    def _():
        pass_on(1 - first)

    for h in range(heads):
        lanes = slice(h * HG_DK, (h + 1) * HG_DK)
        carry_f = srecv[0, h].astype(F32)
        carry_b = srecv[1, h].astype(F32)
        starts_f = []
        for b in range(blocks):
            starts_f.append(carry_f)
            carry_f = carry_f * block_decay[h][0][b] + sf_ref[b, :, lanes]
        starts_b = [None] * blocks
        for b in range(blocks - 1, -1, -1):
            starts_b[b] = carry_b
            carry_b = carry_b * block_decay[h][1][b] + sb_ref[b, :, lanes]
        for b in range(blocks):
            tok = slice(b * BLOCK, (b + 1) * BLOCK)
            o = intra[tok, lanes]
            o = o + mm_nt(qf_ref[tok, lanes], starts_f[b].astype(BF16))
            o = o + mm_nt(qb_ref[tok, lanes], starts_b[b].astype(BF16))
            o = o * lax.rsqrt(jnp.mean(o * o, axis=-1, keepdims=True) + norm_eps) * gain_ref[:, lanes]
            act[tok, lanes] = o.astype(BF16)

    mine = pl.multiple_of(tp * rows, rows)
    theirs = pl.multiple_of((1 - tp) * rows, rows)
    kept_rows = []
    x_copies = []

    def finish(j):
        x_copies[j].wait_recv()
        at = pl.multiple_of(flip_bits(fs, j) * columns, LANES)
        out_ref[:, pl.ds(at, columns)] = (kept_rows[j] + precv[j].astype(F32)).astype(BF16)

    for j in range(n_fs):
        if j == 0:
            for c in own:
                c.wait()
        else:
            for c in relays[j] if j in far else w_copies[j]:
                c.wait_recv()
        away = mm(act[pl.ds(theirs, rows), :width], w1buf[j]) + mm(act[pl.ds(theirs, rows), width:], w2buf[j])
        psend[j] = away.astype(BF16)
        c = remote(psend.at[j], precv.at[j], x_send.at[j], x_recv.at[j], partner)
        c.start()
        x_copies.append(c)
        here = mm(act[pl.ds(mine, rows), :width], w1buf[j]) + mm(act[pl.ds(mine, rows), width:], w2buf[j])
        kept_rows.append(here.astype(BF16).astype(F32))
        if j > 0:
            finish(j - 1)
    finish(n_fs - 1)

    for pieces in list(w_copies.values()) + list(relays.values()):
        for c in pieces:
            c.wait_send()
    for c in l_copies + forwards + x_copies:
        c.wait_send()
    for d in range(2):
        for h in range(heads):
            @pl.when(has_next(d))
            def _():
                link(d, h).wait_send()


def local(
    n_fs,
    n_sp,
    recurrent_query,
    forget_logits,
    recurrent_value,
    forget_floor,
    extra_log_decay,
    recurrent_norm_gain,
    attention_query,
    latent,
    rotary_key,
    latent_norm_gain,
    latent_up_weight,
    recurrent_output_weight,
    attention_output_weight,
):
    span = min(n_sp, widest_span)
    tokens, width = recurrent_query.shape[1:]
    heads = width // HG_DK
    att_heads = attention_query.shape[2] // HEAD
    latent_width = latent.shape[2]
    columns = recurrent_output_weight.shape[1]
    att_width = attention_output_weight.shape[0]
    blocks = tokens // BLOCK
    rows = tokens // 2
    cos_pad, sin_pad, place, swap = rope_constants(span * tokens, att_heads)
    vmem = pl.BlockSpec(memory_space=pltpu.VMEM)
    anywhere = pl.BlockSpec(memory_space=pl.ANY)
    dma = pltpu.SemaphoreType.DMA
    mixed, log_weight = pl.pallas_call(
        functools.partial(kernel, (n_fs, span)),
        out_shape=(
            jax.ShapeDtypeStruct((rows, columns * n_fs), BF16),
            jax.ShapeDtypeStruct((att_heads, tokens), F32),
        ),
        in_specs=[vmem] * 15 + [anywhere] * 2,
        out_specs=(vmem, vmem),
        scratch_shapes=[
            pltpu.VMEM((span, tokens, latent_width + LANES), BF16),
            pltpu.VMEM((2, heads, HG_DK, HG_DK), BF16),
            pltpu.VMEM((2, heads, HG_DK, HG_DK), BF16),
            pltpu.VMEM((n_fs, width, columns), BF16),
            pltpu.VMEM((n_fs, att_width, columns), BF16),
            pltpu.VMEM((n_fs, rows, columns), BF16),
            pltpu.VMEM((n_fs, rows, columns), BF16),
            pltpu.VMEM((span * tokens, att_heads * LANES), BF16),
            pltpu.VMEM((span * tokens, att_heads * LANES), BF16),
            pltpu.VMEM((tokens, width), F32),
            pltpu.VMEM((tokens, width), BF16),
            pltpu.VMEM((tokens, width), BF16),
            pltpu.VMEM((blocks, HG_DK, width), F32),
            pltpu.VMEM((blocks, HG_DK, width), F32),
            pltpu.VMEM((tokens, width + att_width), BF16),
            pltpu.VMEM((2, heads, HG_DK, HG_DK), F32),
            pltpu.VMEM((2, heads, 8, HG_DK), F32),
            dma((span,)), dma((span,)), dma((span,)), dma((span,)), dma((2, heads)), dma((2, heads)),
            dma((2 * n_fs,)), dma((2 * n_fs,)), dma((2 * n_fs,)), dma((2 * n_fs,)),
            dma((n_fs,)), dma((n_fs,)), dma((2,)),
        ],
        compiler_params=pltpu.CompilerParams(
            collective_id=0, has_side_effects=True, vmem_limit_bytes=56 * 2**20
        ),
        name="mixers",
    )(
        recurrent_query[0],
        forget_logits[0],
        recurrent_value[0],
        forget_floor,
        extra_log_decay[0].T,
        recurrent_norm_gain[None],
        attention_query[0],
        latent[0],
        rotary_key[0].T,
        latent_norm_gain[None],
        latent_up_weight,
        jnp.asarray(cos_pad),
        jnp.asarray(sin_pad),
        jnp.asarray(place, BF16),
        jnp.asarray(swap, BF16),
        recurrent_output_weight,
        attention_output_weight,
    )
    return mixed[None], log_weight.T[None]


def solution(mesh):
    placed = (
        P("fs", "sp", "tp"),
        P("fs", "sp", "tp"),
        P("fs", "sp", "tp"),
        P(None, "tp"),
        P("fs", "sp", "tp"),
        P("tp"),
        P("fs", "sp", "tp"),
        P("fs", "sp", None),
        P("fs", "sp", None),
        P(),
        P(),
        P("tp", "fs"),
        P("tp", "fs"),
    )
    return jax.shard_map(
        functools.partial(local, mesh.shape["fs"], mesh.shape["sp"]),
        mesh=mesh,
        in_specs=placed,
        out_specs=(P("fs", ("sp", "tp"), None), P("fs", "sp", "tp")),
        check_vma=False,
    )
```

```python
import functools

import jax
import jax.numpy as jnp
import numpy as np
from jax import lax
from jax.experimental import pallas as pl
from jax.experimental.pallas import tpu as pltpu
from jax.sharding import PartitionSpec as P

HG_DK = 128
NOPE = 64
ROPE = 32
VDIM = 64
HEAD = NOPE + ROPE
LANES = 128
BLOCK = 128

norm_eps = 1e-06
rope_base = 10000.0
widest_span = 8
LOG2_E = 1.4426950408889634

F32 = jnp.float32
BF16 = jnp.bfloat16


def mm(a, b):
    return jnp.dot(a, b, preferred_element_type=F32)


def mm_nt(a, b):
    return lax.dot_general(a, b, (((1,), (1,)), ((), ())), preferred_element_type=F32)


def mm_tn(a, b):
    return lax.dot_general(a, b, (((0,), (0,)), ((), ())), preferred_element_type=F32)


def flip_bits(value, mask):
    bit = 1
    while bit <= mask:
        if mask & bit:
            value = value + bit - 2 * bit * lax.rem(value // bit, 2)
        bit *= 2
    return value


def rope_constants(seq_len, heads):
    half = ROPE // 2
    inverse = (np.float32(rope_base) ** (-np.arange(half, dtype=np.float32) / np.float32(half))).astype(np.float32)
    angles = np.arange(seq_len, dtype=np.float32)[:, None] * inverse[None, :]
    cos_pad = np.zeros((seq_len, LANES), np.float32)
    sin_pad = np.zeros((seq_len, LANES), np.float32)
    cos_pad[:, :NOPE] = 1.0
    cos_pad[:, NOPE:HEAD] = np.tile(np.cos(angles), (1, 2))
    sin_pad[:, NOPE:HEAD] = np.tile(np.sin(angles), (1, 2))
    place = np.zeros((heads * HEAD, heads * LANES), np.float32)
    swap = np.zeros((heads * HEAD, heads * LANES), np.float32)
    for h in range(heads):
        for i in range(HEAD):
            place[h * HEAD + i, h * LANES + i] = 1.0
        for i in range(half):
            a, b = NOPE + i, NOPE + half + i
            swap[h * HEAD + b, h * LANES + a] = -1.0
            swap[h * HEAD + a, h * LANES + b] = 1.0
    return cos_pad, sin_pad, place, swap


def kernel(
    sizes,
    q_ref, f_ref, v_ref, floor_ref, extra_ref, gain_ref, aq_ref, lat_ref, rk_ref,
    lgain_ref, wup_ref, cos_ref, sin_ref, place_ref, swap_ref, w1_ref, w2_ref,
    out_ref, logw_ref,
    lbuf, ssend, srecv, w1buf, w2buf, psend, precv,
    kbuf, vbuf, intra, qf_ref, qb_ref, sf_ref, sb_ref, act, whole_state, whole_decay,
    l_send, l_recv, f_send, f_recv, s_send, s_recv, w_send, w_recv, r_send, r_recv,
    x_send, x_recv, own_sem,
):
    n_fs, span = sizes
    tokens, width = q_ref.shape
    heads = width // HG_DK
    att_heads = aq_ref.shape[1] // HEAD
    up = att_heads * (NOPE + VDIM)
    blocks = tokens // BLOCK
    latent_width = lat_ref.shape[1]
    columns = w1_ref.shape[1]
    rows = tokens // 2

    sp, fs, tp = lax.axis_index("sp"), lax.axis_index("fs"), lax.axis_index("tp")
    place = lax.rem(sp, span)
    base = sp - place

    def sp_peer(j):
        return {"sp": base + lax.rem(place + j, span)}

    def fs_peer(j):
        return {"fs": flip_bits(fs, j)}

    partner = {"tp": 1 - tp}

    barrier = pltpu.get_barrier_semaphore()
    for j in range(1, n_fs):
        pl.semaphore_signal(barrier, inc=1, device_id=fs_peer(j), device_id_type=pl.DeviceIdType.MESH)
    for j in range(1, span):
        pl.semaphore_signal(barrier, inc=1, device_id=sp_peer(j), device_id_type=pl.DeviceIdType.MESH)
    pl.semaphore_signal(barrier, inc=1, device_id=partner, device_id_type=pl.DeviceIdType.MESH)
    pl.semaphore_wait(barrier, n_fs + span - 1)

    def remote(src, dst, send, recv, device):
        return pltpu.make_async_remote_copy(
            src_ref=src, dst_ref=dst, send_sem=send, recv_sem=recv,
            device_id=device, device_id_type=pl.DeviceIdType.MESH,
        )

    parity = lax.rem(place, 2)
    pair = {"sp": base + flip_bits(place, 1)}
    far = [j for j in range(1, n_fs) if j & (j - 1) and span % 2 == 0]
    near = [j for j in range(1, n_fs) if j not in far]
    weights = ((w1_ref, w1buf), (w2_ref, w2buf))

    def half_rows(ref):
        size = ref.shape[-2] // 2
        return pl.ds(pl.multiple_of(parity * size, size), size)

    w_copies = {}
    for j in far + near:
        pieces = []
        for k, (src, dst) in enumerate(weights):
            there = dst.at[j]
            if j in far:
                src, there = src.at[half_rows(src)], there.at[half_rows(dst)]
            c = remote(src, there, w_send.at[2 * j + k], w_recv.at[2 * j + k], fs_peer(j))
            c.start()
            pieces.append(c)
        w_copies[j] = pieces
    relays = {j: [
        remote(dst.at[j, half_rows(dst)], dst.at[j, half_rows(dst)],
               r_send.at[2 * j + k], r_recv.at[2 * j + k], pair)
        for k, (_, dst) in enumerate(weights)
    ] for j in far}
    own = (
        pltpu.make_async_copy(w1_ref, w1buf.at[0], own_sem.at[0]),
        pltpu.make_async_copy(w2_ref, w2buf.at[0], own_sem.at[1]),
    )
    for c in own:
        c.start()

    offset = pl.multiple_of(place * tokens, tokens)
    cos = cos_ref[pl.ds(offset, tokens), :]
    sin = sin_ref[pl.ds(offset, tokens), :]
    lat = lat_ref[...].astype(F32)
    normed = lat * lax.rsqrt(jnp.mean(lat * lat, axis=-1, keepdims=True) + norm_eps) * lgain_ref[...]
    lbuf[0, :, :latent_width] = normed.astype(BF16)
    rk = rk_ref[...]
    rotated = mm_tn(rk, place_ref[NOPE:HEAD, :LANES]) * cos + mm_tn(rk, swap_ref[NOPE:HEAD, :LANES]) * sin
    lbuf[0, :, latent_width:] = rotated.astype(BF16)
    my_rows = pl.ds(pl.multiple_of(tp * rows, rows), rows)
    l_copies = []
    for j in range(1, span):
        c = remote(lbuf.at[0, my_rows], lbuf.at[j, my_rows], l_send.at[j], l_recv.at[j], sp_peer(j))
        c.start()
        l_copies.append(c)

    row = lax.broadcasted_iota(jnp.int32, (BLOCK, BLOCK), 0)
    col = lax.broadcasted_iota(jnp.int32, (BLOCK, BLOCK), 1)
    lower = row >= col
    upper = row <= col
    tri = (jnp.where(lower, 1.0, 0.0).astype(BF16), jnp.where(upper, 1.0, 0.0).astype(BF16))
    spikes = lax.dot_general(
        extra_ref[...],
        jnp.where(
            lax.broadcasted_iota(jnp.int32, (heads, width), 0)
            == lax.broadcasted_iota(jnp.int32, (heads, width), 1) // HG_DK, 1.0, 0.0),
        (((0,), (0,)), ((), ())), precision=lax.Precision.HIGHEST, preferred_element_type=F32)
    block_decay = [[[None] * blocks for _ in range(2)] for _ in range(heads)]
    for h in range(heads):
        lanes = slice(h * HG_DK, (h + 1) * HG_DK)
        for b in range(blocks):
            tok = slice(b * BLOCK, (b + 1) * BLOCK)
            q = q_ref[tok, lanes].astype(F32)
            gate = f_ref[tok, lanes].astype(F32)
            v = v_ref[tok, lanes]
            miss = 1.0 / (1.0 + jnp.exp(gate))
            spike = spikes[tok, lanes]
            scores = None
            for d in range(2):
                keyed = (1.0 - floor_ref[d : d + 1, lanes]) * miss
                decay = jnp.log1p(-keyed) + spike
                hi = decay.astype(BF16)
                lo = (decay - hi.astype(F32)).astype(BF16)
                run = mm(tri[d], hi) + mm(tri[d], lo)
                mid_at = BLOCK // 2 - 1 if d == 0 else BLOCK // 2
                end_at = BLOCK - 1 if d == 0 else 0
                mid = run[mid_at : mid_at + 1]
                end = run[end_at : end_at + 1]
                grow = jnp.exp(run - mid)
                qd = q * grow
                kd = keyed * jnp.exp(mid - run)
                s = mm_nt(qd.astype(BF16), kd.astype(BF16))
                s = jnp.where(lower if d == 0 else upper, s, 0.0)
                scores = s if scores is None else scores + s
                cross = qf_ref if d == 0 else qb_ref
                cross[tok, lanes] = (qd * jnp.exp(mid)).astype(BF16)
                state = mm_tn(v, (kd * jnp.exp(end - mid)).astype(BF16))
                keep = sf_ref if d == 0 else sb_ref
                keep[b, :, lanes] = state
                block_decay[h][d][b] = jnp.exp(end)
            intra[tok, lanes] = mm(scores.astype(BF16), v)
        for d in range(2):
            keep = sf_ref if d == 0 else sb_ref
            order = range(blocks) if d == 0 else range(blocks - 1, -1, -1)
            total, decay_all = None, None
            for b in order:
                one = keep[b, :, lanes]
                dec = block_decay[h][d][b]
                total = one if total is None else total * dec + one
                decay_all = dec if decay_all is None else decay_all * dec
            whole_state[d, h] = total
            whole_decay[d, h] = jnp.broadcast_to(decay_all, (8, HG_DK))

    first = jnp.where(2 * place < span, 0, 1)

    def link(d, h):
        towards = jnp.clip(place + 1 - 2 * d, 0, span - 1)
        return remote(ssend.at[d, h], srecv.at[d, h], s_send.at[d, h], s_recv.at[d, h],
                      {"sp": base + towards})

    def has_previous(d):
        return jnp.where(d == 0, place, span - 1 - place) > 0

    def has_next(d):
        return jnp.where(d == 0, span - 1 - place, place) > 0

    def pass_on(d):
        for h in range(heads):
            @pl.when(has_previous(d))
            def _():
                link(d, h).wait_recv()

            @pl.when(jnp.logical_not(has_previous(d)))
            def _():
                srecv[d, h] = jnp.zeros((HG_DK, HG_DK), BF16)

            @pl.when(has_next(d))
            def _():
                reached = srecv[d, h].astype(F32) * whole_decay[d, h, 0:1] + whole_state[d, h]
                ssend[d, h] = reached.astype(BF16)
                link(d, h).start()

    for j in far:
        for c, r in zip(w_copies[j], relays[j]):
            c.wait_recv()
            r.start()

    pass_on(first)

    forwards = []
    for j in range(1, span):
        l_copies[j - 1].wait_recv()
        c = remote(lbuf.at[j, my_rows], lbuf.at[j, my_rows], f_send.at[j], f_recv.at[j], partner)
        c.start()
        forwards.append(c)

    @pl.when(has_next(1 - first))
    def _():
        pass_on(1 - first)

    tp_up = pl.multiple_of(tp * up, LANES)
    wup = wup_ref[:, pl.ds(tp_up, up)]
    lane = lax.broadcasted_iota(jnp.int32, (tokens, LANES), 1)
    for j in range(span):
        if j > 0:
            forwards[j - 1].wait_recv()
        keys = slice(j * tokens, (j + 1) * tokens)
        expanded = mm(lbuf[j, :, :latent_width], wup)
        rot = lbuf[j, :, latent_width:].astype(F32)
        vbuf[keys, :] = expanded.astype(BF16)
        for h in range(att_heads):
            lanes = slice(h * LANES, (h + 1) * LANES)
            kbuf[keys, lanes] = jnp.where(lane < NOPE, expanded[:, lanes], rot).astype(BF16)
    aq = aq_ref[...]
    scale = HEAD ** (-0.5)
    logw = jnp.zeros((tokens, LANES), F32)
    kept = None
    for h in range(att_heads):
        lanes = slice(h * LANES, (h + 1) * LANES)
        query = mm(aq, place_ref[:, lanes]) * cos + mm(aq, swap_ref[:, lanes]) * sin
        scores = mm_nt(query.astype(BF16), kbuf[:, lanes])
        top = jnp.max(scores, axis=-1, keepdims=True)
        peak = top * scale
        weights = jnp.exp2((scores - top) * (scale * LOG2_E))
        totals = jnp.sum(weights, axis=-1, keepdims=True)
        result = mm(weights.astype(BF16), vbuf[:, lanes]) / totals
        logw = jnp.where(lane == h, peak + jnp.log(totals), logw)
        if h % 2 == 0:
            kept = pltpu.roll(result, VDIM, 1)
        else:
            at = width + (h // 2) * LANES
            act[:, at : at + LANES] = jnp.where(lane < VDIM, kept, result).astype(BF16)
    logw_ref[...] = jnp.transpose(logw)[:att_heads]

    @pl.when(jnp.logical_not(has_next(1 - first)))
    def _():
        pass_on(1 - first)

    for h in range(heads):
        lanes = slice(h * HG_DK, (h + 1) * HG_DK)
        carry_f = srecv[0, h].astype(F32)
        carry_b = srecv[1, h].astype(F32)
        starts_f = []
        for b in range(blocks):
            starts_f.append(carry_f)
            carry_f = carry_f * block_decay[h][0][b] + sf_ref[b, :, lanes]
        starts_b = [None] * blocks
        for b in range(blocks - 1, -1, -1):
            starts_b[b] = carry_b
            carry_b = carry_b * block_decay[h][1][b] + sb_ref[b, :, lanes]
        for b in range(blocks):
            tok = slice(b * BLOCK, (b + 1) * BLOCK)
            o = intra[tok, lanes]
            o = o + mm_nt(qf_ref[tok, lanes], starts_f[b].astype(BF16))
            o = o + mm_nt(qb_ref[tok, lanes], starts_b[b].astype(BF16))
            o = o * lax.rsqrt(jnp.mean(o * o, axis=-1, keepdims=True) + norm_eps) * gain_ref[:, lanes]
            act[tok, lanes] = o.astype(BF16)

    mine = pl.multiple_of(tp * rows, rows)
    theirs = pl.multiple_of((1 - tp) * rows, rows)
    kept_rows = {}
    x_copies = {}

    def part(at, j, k):
        rows_at = pl.ds(at, rows)
        if k == 0:
            return mm(act[rows_at, :width], w1buf[j])
        return mm(act[rows_at, width:], w2buf[j])

    def arrive(j, k):
        if j == 0:
            own[k].wait()
        else:
            (relays[j] if j in far else w_copies[j])[k].wait_recv()

    def exchange(j, away, here):
        psend[j] = away.astype(BF16)
        c = remote(psend.at[j], precv.at[j], x_send.at[j], x_recv.at[j], partner)
        c.start()
        x_copies[j] = c
        kept_rows[j] = (here if here is not None else part(mine, j, 0) + part(mine, j, 1)).astype(BF16).astype(F32)

    def finish(j):
        x_copies[j].wait_recv()
        at = pl.multiple_of(flip_bits(fs, j) * columns, LANES)
        out_ref[:, pl.ds(at, columns)] = (kept_rows[j] + precv[j].astype(F32)).astype(BF16)

    for j in [0] + far:
        arrive(j, 0)
        arrive(j, 1)
        exchange(j, part(theirs, j, 0) + part(theirs, j, 1), None)
    begun = {}
    for j in near:
        arrive(j, 0)
        begun[j] = (part(theirs, j, 0), part(mine, j, 0))
    for j in [0] + far:
        finish(j)
    for j in near:
        arrive(j, 1)
        exchange(j, begun[j][0] + part(theirs, j, 1), begun[j][1] + part(mine, j, 1))
    for j in near:
        finish(j)

    for pieces in list(w_copies.values()) + list(relays.values()):
        for c in pieces:
            c.wait_send()
    for c in l_copies + forwards + list(x_copies.values()):
        c.wait_send()
    for d in range(2):
        for h in range(heads):
            @pl.when(has_next(d))
            def _():
                link(d, h).wait_send()


def local(
    n_fs,
    n_sp,
    recurrent_query,
    forget_logits,
    recurrent_value,
    forget_floor,
    extra_log_decay,
    recurrent_norm_gain,
    attention_query,
    latent,
    rotary_key,
    latent_norm_gain,
    latent_up_weight,
    recurrent_output_weight,
    attention_output_weight,
):
    span = min(n_sp, widest_span)
    tokens, width = recurrent_query.shape[1:]
    heads = width // HG_DK
    att_heads = attention_query.shape[2] // HEAD
    latent_width = latent.shape[2]
    columns = recurrent_output_weight.shape[1]
    att_width = attention_output_weight.shape[0]
    blocks = tokens // BLOCK
    rows = tokens // 2
    cos_pad, sin_pad, place, swap = rope_constants(span * tokens, att_heads)
    vmem = pl.BlockSpec(memory_space=pltpu.VMEM)
    anywhere = pl.BlockSpec(memory_space=pl.ANY)
    dma = pltpu.SemaphoreType.DMA
    mixed, log_weight = pl.pallas_call(
        functools.partial(kernel, (n_fs, span)),
        out_shape=(
            jax.ShapeDtypeStruct((rows, columns * n_fs), BF16),
            jax.ShapeDtypeStruct((att_heads, tokens), F32),
        ),
        in_specs=[vmem] * 15 + [anywhere] * 2,
        out_specs=(vmem, vmem),
        scratch_shapes=[
            pltpu.VMEM((span, tokens, latent_width + LANES), BF16),
            pltpu.VMEM((2, heads, HG_DK, HG_DK), BF16),
            pltpu.VMEM((2, heads, HG_DK, HG_DK), BF16),
            pltpu.VMEM((n_fs, width, columns), BF16),
            pltpu.VMEM((n_fs, att_width, columns), BF16),
            pltpu.VMEM((n_fs, rows, columns), BF16),
            pltpu.VMEM((n_fs, rows, columns), BF16),
            pltpu.VMEM((span * tokens, att_heads * LANES), BF16),
            pltpu.VMEM((span * tokens, att_heads * LANES), BF16),
            pltpu.VMEM((tokens, width), F32),
            pltpu.VMEM((tokens, width), BF16),
            pltpu.VMEM((tokens, width), BF16),
            pltpu.VMEM((blocks, HG_DK, width), F32),
            pltpu.VMEM((blocks, HG_DK, width), F32),
            pltpu.VMEM((tokens, width + att_width), BF16),
            pltpu.VMEM((2, heads, HG_DK, HG_DK), F32),
            pltpu.VMEM((2, heads, 8, HG_DK), F32),
            dma((span,)), dma((span,)), dma((span,)), dma((span,)), dma((2, heads)), dma((2, heads)),
            dma((2 * n_fs,)), dma((2 * n_fs,)), dma((2 * n_fs,)), dma((2 * n_fs,)),
            dma((n_fs,)), dma((n_fs,)), dma((2,)),
        ],
        compiler_params=pltpu.CompilerParams(
            collective_id=0, has_side_effects=True, vmem_limit_bytes=56 * 2**20
        ),
        name="mixers",
    )(
        recurrent_query[0],
        forget_logits[0],
        recurrent_value[0],
        forget_floor,
        extra_log_decay[0].T,
        recurrent_norm_gain[None],
        attention_query[0],
        latent[0],
        rotary_key[0].T,
        latent_norm_gain[None],
        latent_up_weight,
        jnp.asarray(cos_pad),
        jnp.asarray(sin_pad),
        jnp.asarray(place, BF16),
        jnp.asarray(swap, BF16),
        recurrent_output_weight,
        attention_output_weight,
    )
    return mixed[None], log_weight.T[None]


def solution(mesh):
    placed = (
        P("fs", "sp", "tp"),
        P("fs", "sp", "tp"),
        P("fs", "sp", "tp"),
        P(None, "tp"),
        P("fs", "sp", "tp"),
        P("tp"),
        P("fs", "sp", "tp"),
        P("fs", "sp", None),
        P("fs", "sp", None),
        P(),
        P(),
        P("tp", "fs"),
        P("tp", "fs"),
    )
    return jax.shard_map(
        functools.partial(local, mesh.shape["fs"], mesh.shape["sp"]),
        mesh=mesh,
        in_specs=placed,
        out_specs=(P("fs", ("sp", "tp"), None), P("fs", "sp", "tp")),
        check_vma=False,
    )
```
